32 devices in a mesh: sp: 4 (over y, core), dp: 8 (over z, x).
Axes of the slice: x: 2, y: 2, z: 4, core: 2. Of those that a mesh axis runs over, the one named last changes fastest.
Arguments:
- q_latent: bfloat16 [8, 512, 512], P('dp', 'sp'), may hold values from -70 to 70
- kv_latent: bfloat16 [8, 512, 512], P('dp', 'sp'), may hold values from -70 to 70
- rope_key: bfloat16 [8, 512, 64], P('dp', 'sp'), may hold values from -370 to 370
- w_query: bfloat16 [512, 3072], P(None, 'dp'), may hold values from -0.25 to 0.25
- w_keyval: bfloat16 [512, 4096], P(None, 'sp'), may hold values from -0.25 to 0.25
- w_out: bfloat16 [2048, 2048], replicated, may hold values from -0.125 to 0.125
- query_gain: bfloat16 [512], replicated, may hold values from 0.099609375 to 1.8984375
- latent_gain: bfloat16 [512], replicated, may hold values from 0.099609375 to 1.8984375
- out_gain: bfloat16 [2048], replicated, may hold values from 0.099609375 to 1.8984375
Outputs:
- output: bfloat16 [8, 512, 2048], P('dp', 'sp')
The draws below stay inside these ranges and needn't reach their ends.
All inputs are finite; a program needn't handle non-finite values.
Results may differ from the reference program's by a relative error of at most 0.03.
The reference program's roundings to bfloat16 on the way (of `query_norm`, `queries`, `latent_norm`, `keyval`, `rope_turned`, `weights`, `attended` and `mixed_norm`) count: a program that leaves them out, or rounds other values in their place, can miss the bound.
Values may be sent and summed in bfloat16 or wider, within the bound.
A program may use at most 64 MiB of HBM per device.

```python
import math
import jax
import jax.numpy as jnp
from jax import lax

D = 2048
H = 16
QR = 512
KR = 512
NOPE = 128
ROPE = 64
VDIM = 128
SEQ_LEN = 512
SEQS = 8


def scaled_latent_draw(key, width):
    base_key, channel_key, row_key = jax.random.split(key, 3)
    array_shape = (SEQS, SEQ_LEN, width)
    base_draw = jnp.clip(jax.random.normal(base_key, array_shape, jnp.float32), -5.0, 5.0)
    channel = jnp.exp(jax.random.uniform(channel_key, (width,), jnp.float32, math.log(0.3), math.log(3.0)))
    row_scale = jnp.exp(jax.random.uniform(row_key, (SEQS, SEQ_LEN, 1), jnp.float32, math.log(0.3), math.log(3.0)))
    return base_draw * channel * row_scale


def draw_q_latent(key, part):
    return scaled_latent_draw(jax.random.fold_in(key, 11), QR).astype(jnp.bfloat16)


def draw_kv_latent(key, part):
    return scaled_latent_draw(jax.random.fold_in(key, 12), KR).astype(jnp.bfloat16)


def draw_rope_key(key, part):
    base_key = jax.random.fold_in(jax.random.fold_in(key, 13), 0)
    array_shape = (SEQS, SEQ_LEN, ROPE)
    result_draw = jnp.clip(jax.random.normal(base_key, array_shape, jnp.float32), -5.0, 5.0)
    return result_draw.astype(jnp.bfloat16)


def steps_of(own_key, extent, cuts, least, largest):
    gain = 1.0
    for dim, parts in cuts:
        draws = jax.random.uniform(jax.random.fold_in(jax.random.fold_in(own_key, 6), dim), (parts,), jnp.float32, least / len(cuts), largest / len(cuts))
        gain = gain * jnp.repeat(jnp.exp(draws), extent[dim] // parts).reshape((-1,) + (1,) * (len(extent) - 1 - dim))
    return gain


def noise(own_key, shape, scale, limit, cuts=(), kind=jnp.bfloat16):
    values = scale * jax.random.normal(own_key, shape, jnp.float32)
    if cuts:
        values = values * steps_of(own_key, shape, cuts, -0.22, 0.18)
    return jnp.clip(values, -limit, limit).astype(kind)


def setup_inputs(seed: int = 0) -> dict:
    keys = jax.random.split(jax.random.key(seed), 10)
    return {
        "q_latent": draw_q_latent(jax.random.fold_in(keys[9], 71), 0),
        "kv_latent": draw_kv_latent(jax.random.fold_in(keys[9], 71), 0),
        "rope_key": draw_rope_key(jax.random.fold_in(keys[9], 71), 0),
        "w_query": noise(keys[3], (QR, H * (NOPE + ROPE)), QR ** -0.5, 0.25, ((1, 8),)),
        "w_keyval": noise(keys[4], (KR, H * (NOPE + VDIM)), KR ** -0.5, 0.25, ((1, 4),)),
        "w_out": noise(keys[5], (H * VDIM, D), (H * VDIM) ** -0.5, 0.125),
        "query_gain": jnp.clip(1.0 + 0.18 * jax.random.normal(keys[6], (QR,), jnp.float32), 0.099609375, 1.8984375).astype(jnp.bfloat16),
        "latent_gain": jnp.clip(1.0 + 0.18 * jax.random.normal(keys[7], (KR,), jnp.float32), 0.099609375, 1.8984375).astype(jnp.bfloat16),
        "out_gain": jnp.clip(1.0 + 0.18 * jax.random.normal(keys[8], (H * VDIM,), jnp.float32), 0.099609375, 1.8984375).astype(jnp.bfloat16),
    }


def normalize(row_values, gain_vector):
    widened = row_values.astype(jnp.float32)
    return widened * lax.rsqrt(lax.optimization_barrier(jnp.mean(widened * widened, axis=-1, keepdims=True)) + 1e-05) * gain_vector.astype(jnp.float32)

def angles_for(positions, rope_width):
    half_width = rope_width // 2
    inverse = 10000.0 ** (-jnp.arange(half_width, dtype=jnp.float32) / half_width)
    return positions.astype(jnp.float32)[:, None] * inverse[None, :]

def turn(vectors, angles):
    half_width = vectors.shape[-1] // 2
    cosine = jnp.cos(angles)
    sine_value = jnp.sin(angles)
    low_half = vectors[..., :half_width]
    high_half = vectors[..., half_width:]
    return jnp.concatenate([low_half * cosine - high_half * sine_value, high_half * cosine + low_half * sine_value], axis=-1)

def one_sequence(query_latent, kv_rows, rope_rows, w_query, w_keyval, w_out, query_gain, latent_gain, out_gain):
    length = query_latent.shape[0]
    positions = jnp.arange(length, dtype=jnp.int32)
    angles = angles_for(positions, ROPE)
    query_norm = normalize(query_latent, query_gain).astype(jnp.bfloat16)
    query_raw = jnp.dot(query_norm, w_query, preferred_element_type=jnp.float32).reshape(length, H, NOPE + ROPE)
    queries = jnp.concatenate([query_raw[..., :NOPE], turn(query_raw[..., NOPE:], angles[:, None, :])], axis=-1).astype(jnp.bfloat16)
    queries = lax.optimization_barrier(queries)
    latent_norm = normalize(kv_rows, latent_gain).astype(jnp.bfloat16)
    keyval = jnp.dot(latent_norm, w_keyval, preferred_element_type=jnp.float32).astype(jnp.bfloat16)
    keyval = lax.optimization_barrier(keyval).reshape(length, H, NOPE + VDIM)
    rope_turned = turn(rope_rows.astype(jnp.float32), angles).astype(jnp.bfloat16)
    rope_turned = lax.optimization_barrier(rope_turned)
    key_rows = jnp.concatenate([keyval[..., :NOPE], jnp.broadcast_to(rope_turned[:, None, :], (length, H, ROPE))], axis=-1)
    value_rows = keyval[..., NOPE:]
    block_rows = min(512, length)
    score_scale = (NOPE + ROPE) ** (-0.5)
    pieces = []
    for block_index in range(length // block_rows):
        block_start = block_index * block_rows
        block_stop = block_start + block_rows
        scores = jnp.einsum('qhd,khd->hqk', queries[block_start:block_stop].astype(jnp.float32), key_rows[:block_stop].astype(jnp.float32)) * score_scale
        allowed = jnp.arange(block_stop)[None, :] <= (block_start + jnp.arange(block_rows))[:, None]
        scores = jnp.where(allowed[None], scores, -jnp.inf)
        row_top = lax.optimization_barrier(jnp.max(scores, axis=-1, keepdims=True))
        exponent = jnp.exp(scores - row_top)
        row_total = lax.optimization_barrier(jnp.sum(exponent, axis=-1))
        weights = lax.optimization_barrier(exponent.astype(jnp.bfloat16))
        summed = jnp.einsum('hqk,khd->qhd', weights.astype(jnp.float32), value_rows[:block_stop].astype(jnp.float32))
        pieces.append((summed / jnp.transpose(row_total)[:, :, None]).astype(jnp.bfloat16))
    attended = lax.optimization_barrier(jnp.concatenate(pieces, axis=0)).reshape(length, H * VDIM)
    mixed_norm = normalize(attended, out_gain).astype(jnp.bfloat16)
    return jnp.dot(mixed_norm, w_out, preferred_element_type=jnp.float32).astype(jnp.bfloat16)

def reference(q_latent, kv_latent, rope_key, w_query, w_keyval, w_out, query_gain, latent_gain, out_gain):

    def per_sequence(inputs):
        return one_sequence(inputs[0], inputs[1], inputs[2], w_query, w_keyval, w_out, query_gain, latent_gain, out_gain)
    return lax.map(per_sequence, (q_latent, kv_latent, rope_key))
```

```python
import functools

import jax
import jax.numpy as jnp
import numpy as np
from jax import lax
from jax.experimental import pallas as pl
from jax.experimental.pallas import tpu as pltpu
from jax.sharding import PartitionSpec as P

H = 16
NOPE = 128
ROPE = 64
VDIM = 128
HEAD = NOPE + ROPE
MESH = pl.DeviceIdType.MESH
F32 = jnp.float32
BF16 = jnp.bfloat16


def turn_table(length):
    half = ROPE // 2
    inverse = np.float32(10000.0) ** (-np.arange(half, dtype=np.float32) / np.float32(half))
    angles = np.arange(length, dtype=np.float32)[:, None] * inverse[None, :].astype(np.float32)
    angles = angles.astype(np.float64)
    cosine, sine = np.cos(angles), np.sin(angles)
    return np.concatenate([cosine, cosine, sine, sine], axis=1).astype(np.float32)


def spread_matrix(rows, row_start, head):
    g = lax.broadcasted_iota(jnp.int32, (rows, 256), 0) + row_start
    f = lax.broadcasted_iota(jnp.int32, (rows, 256), 1)
    source = jnp.where(f < HEAD, f, jnp.where(f < HEAD + 32, f - 32, f - 96)) + head * HEAD
    sign = jnp.where((f >= HEAD) & (f < HEAD + 32), -1.0, 1.0)
    return jnp.where(g == source, sign, 0.0).astype(BF16)


def rope_matrix():
    r = lax.broadcasted_iota(jnp.int32, (ROPE, 128), 0)
    f = lax.broadcasted_iota(jnp.int32, (ROPE, 128), 1)
    source = jnp.where(f < 64, f, jnp.where(f < 96, f - 32, f - 96))
    sign = jnp.where((f >= 64) & (f < 96), -1.0, 1.0)
    return jnp.where(r == source, sign, 0.0).astype(BF16)


def scaled_rows(values, gain):
    wide = values.astype(F32)
    mean = jnp.mean(wide * wide, axis=-1, keepdims=True)
    return (wide * lax.rsqrt(mean + 1e-05) * gain).astype(BF16)


def kernel(
    geometry,
    q_ref, kv_ref, rope_ref, wq_ref, wkv_ref, wout_ref, table_ref, qg_ref, lg_ref, og_ref,
    out_ref,
    qall, kvall, ropeall, wqall, wkv, wout, table, wp, qn, qs, ks, vs, att_out, att_in, acc,
    local_sem, gat_send, gat_recv, fwd_send, w_send, w_recv, att_send, att_recv,
):
    n, m, X, k, chunks, local_heads = geometry
    Z = m // X
    rows = q_ref.shape[1]
    n_chips = n // 2
    i = lax.axis_index("sp")
    j = lax.axis_index("dp")
    core = lax.rem(i, 2)
    chip = lax.div(i, 2)
    partner = i + 1 - 2 * core
    z = lax.div(j, X)
    x = lax.rem(j, X)
    first = i * k
    owns = (j >= first) & (j < first + k)

    gathered = ((kv_ref.at[0], kvall), (rope_ref.at[0], ropeall), (q_ref.at[0], qall))
    own_copies = [
        pltpu.make_async_copy(src, dst.at[i], local_sem.at[a]) for a, (src, dst) in enumerate(gathered)
    ]
    wq_copy = pltpu.make_async_copy(wq_ref, wqall.at[lax.rem(j, k)], local_sem.at[3])
    wkv_copy = pltpu.make_async_copy(wkv_ref, wkv, local_sem.at[4])
    table_copy = pltpu.make_async_copy(table_ref, table, local_sem.at[5])
    wout_copy = pltpu.make_async_copy(wout_ref, wout, local_sem.at[6])

    @pl.when(owns)
    def _():
        wq_copy.start()

    for copy in own_copies:
        copy.start()
    wkv_copy.start()
    table_copy.start()
    wout_copy.start()

    barrier = pltpu.get_barrier_semaphore()
    for d in range(1, n):
        pl.semaphore_signal(
            barrier, inc=1, device_id={"sp": lax.rem(i + d, n)}, device_id_type=MESH
        )
    sides = ((z < Z - 1, j + X), (z > 0, j - X), (x < X - 1, j + 1), (x > 0, j - 1))
    count = n - 1
    for present, target in sides:
        @pl.when(present)
        def _(target=target):
            pl.semaphore_signal(barrier, inc=1, device_id={"dp": target}, device_id_type=MESH)
        count = count + jnp.where(present, 1, 0)
    pl.semaphore_wait(barrier, count)

    step_rows = wqall.shape[1] // chunks

    def relay_parts(slot, c):
        owner = first + slot
        zo, xo = lax.div(owner, X), lax.rem(owner, X)
        part = wqall.at[slot, pl.ds(c * step_rows, step_rows)]
        in_column = x == xo
        conditions = (
            in_column & (z >= zo) & (z < Z - 1),
            in_column & (z <= zo) & (z > 0),
            (x >= xo) & (x < X - 1),
            (x <= xo) & (x > 0),
        )
        copies = [
            pltpu.make_async_remote_copy(
                src_ref=part, dst_ref=part,
                send_sem=w_send.at[side, slot, c], recv_sem=w_recv.at[slot, c],
                device_id={"dp": sides[side][1]}, device_id_type=MESH,
            )
            for side in range(4)
        ]
        return owner, conditions, copies

    def relay(slot, c):
        owner, conditions, copies = relay_parts(slot, c)

        @pl.when(owner != j)
        def _():
            copies[0].wait_recv()

        for condition, copy in zip(conditions, copies):
            @pl.when(condition)
            def _(copy=copy):
                copy.start()

    def relay_finish(slot, c):
        _, conditions, copies = relay_parts(slot, c)
        for condition, copy in zip(conditions, copies):
            @pl.when(condition)
            def _(copy=copy):
                copy.wait_send()

    if k == X:
        columns = [lax.rem(x + t, k) for t in range(k)]
        events = []
        for c in range(chunks + k - 1):
            for t in range(k):
                if 0 <= c - t < chunks:
                    events.append((columns[t], c - t))
    else:
        events = [(slot, c) for c in range(chunks) for slot in range(k)]
    events_left = list(events)

    def relay_some(number):
        for _ in range(min(number, len(events_left))):
            relay(*events_left.pop(0))

    def gather_copy(a, slot, sem, target):
        dst = gathered[a][1]
        return pltpu.make_async_remote_copy(
            src_ref=dst.at[slot], dst_ref=dst.at[slot],
            send_sem=sem, recv_sem=gat_recv.at[a, slot],
            device_id={"sp": target}, device_id_type=MESH,
        )

    sends = []

    @pl.when(owns)
    def _():
        wq_copy.wait()

    for a in range(3):
        own_copies[a].wait()
        for d in range(1, n_chips):
            target = 2 * lax.rem(chip + d, n_chips) + core
            sends.append(gather_copy(a, i, gat_send.at[a, d], target))
            sends[-1].start()
    for a in range(3):
        sends.append(gather_copy(a, i, gat_send.at[a, 0], partner))
        sends[-1].start()

    def far_slot(d):
        return 2 * lax.rem(chip + n_chips - d, n_chips) + core

    def forward(a, d):
        slot = far_slot(d)
        copy = gather_copy(a, slot, fwd_send.at[a, d - 1], partner)
        copy.wait_recv()
        copy.start()
        sends.append(copy)

    def arrive(a, slot):
        gather_copy(a, slot, gat_send.at[a, 0], partner).wait_recv()

    lane = lax.broadcasted_iota(jnp.int32, (rows, 128), 1)
    latent_gain = lg_ref[...].astype(F32)
    query_gain = qg_ref[...].astype(F32)
    turner = rope_matrix()

    def keyval(slot):
        at = pl.ds(pl.multiple_of(slot * rows, rows), rows)
        both = jnp.dot(
            scaled_rows(kvall[slot], latent_gain), wkv[...], preferred_element_type=F32
        ).astype(BF16)
        pair = jnp.dot(ropeall[slot], turner, preferred_element_type=F32) * table[at, :]
        pair = pair + pltpu.roll(pair, 64, 1)
        turned = jnp.where(lane < 64, pair, 0.0).astype(BF16)
        for h in range(local_heads):
            base = h * (NOPE + VDIM)
            ks[h, at, 0:NOPE] = both[:, base:base + NOPE]
            ks[h, at, NOPE:256] = turned
            vs[h, at, :] = both[:, base + NOPE:base + NOPE + VDIM]

    def query_rows(slot):
        at = pl.ds(pl.multiple_of(slot * rows, rows), rows)
        qn[at, :] = scaled_rows(qall[slot], query_gain)

    relay_some(k + 1)
    wkv_copy.wait()
    table_copy.wait()
    keyval(i)
    relay_some(1)
    query_rows(i)
    relay_some(1)
    arrive(0, partner)
    arrive(1, partner)
    keyval(partner)
    relay_some(1)
    for d in range(1, n_chips):
        forward(0, d)
        forward(1, d)
        keyval(far_slot(d))
        relay_some(1)
    arrive(2, partner)
    query_rows(partner)
    relay_some(2)
    for d in range(1, n_chips):
        other = far_slot(d) + 1 - 2 * core
        arrive(0, other)
        arrive(1, other)
        keyval(other)
        relay_some(2)
    for d in range(1, n_chips):
        forward(2, d)
        query_rows(far_slot(d))
        relay_some(2)
    for d in range(1, n_chips):
        other = far_slot(d) + 1 - 2 * core
        arrive(2, other)
        query_rows(other)
    relay_some(len(events_left))

    width = wqall.shape[2]
    for h in range(local_heads):
        total = None
        for s in range(k):
            if (s + 1) * width <= h * HEAD or s * width >= (h + 1) * HEAD:
                continue
            term = jnp.dot(
                wqall[s], spread_matrix(width, s * width, h), preferred_element_type=F32
            )
            total = term if total is None else total + term
        wp[h] = total.astype(BF16)
        raw = jnp.dot(qn[...], wp[h], preferred_element_type=F32)
        qs[h, :, 0:NOPE] = raw[:, 0:NOPE].astype(BF16)
        pair = raw[:, NOPE:256] * table[...]
        qs[h, :, NOPE:256] = (pair + pltpu.roll(pair, 64, 1)).astype(BF16)

    power = HEAD ** (-0.5) * float(np.log2(np.e))
    causal = lax.broadcasted_iota(jnp.int32, (rows, rows), 1) <= lax.broadcasted_iota(
        jnp.int32, (rows, rows), 0
    )

    def attend(b):
        stop = (b + 1) * rows
        for h in range(local_heads):
            scores = lax.dot_general(
                qs[h, b * rows:stop, :], ks[h, 0:stop, :], (((1,), (1,)), ((), ())),
                preferred_element_type=F32,
            )
            last = jnp.where(causal, scores[:, b * rows:], -jnp.inf)
            if b:
                scores = jnp.concatenate([scores[:, :b * rows], last], axis=1)
            else:
                scores = last
            top = jnp.max(scores, axis=-1, keepdims=True)
            weights = jnp.exp2((scores - top) * power)
            row_total = jnp.sum(weights, axis=-1, keepdims=True)
            summed = jnp.dot(weights.astype(BF16), vs[h, 0:stop, :], preferred_element_type=F32)
            att_out[b, :, h * VDIM:(h + 1) * VDIM] = (summed / row_total).astype(BF16)

    def att_copy(b):
        return pltpu.make_async_remote_copy(
            src_ref=att_out.at[b], dst_ref=att_in.at[i],
            send_sem=att_send.at[b], recv_sem=att_recv.at[i],
            device_id={"sp": b}, device_id_type=MESH,
        )

    for b in range(n):
        @pl.when(chip != b // 2)
        def _(b=b):
            attend(b)
            att_copy(b).start()
    for b in range(n):
        @pl.when(partner == b)
        def _(b=b):
            attend(b)
            att_copy(b).start()
    for b in range(n):
        @pl.when(i == b)
        def _(b=b):
            attend(b)

    group = local_heads * VDIM
    wout_copy.wait()
    squares = None
    order = [partner]
    for d in range(1, n_chips):
        order += [far_slot(d), far_slot(d) + 1 - 2 * core]
    for t, s in enumerate([i] + order):
        if t:
            pltpu.make_async_remote_copy(
                src_ref=att_in.at[s], dst_ref=att_in.at[s],
                send_sem=att_send.at[0], recv_sem=att_recv.at[s],
                device_id={"sp": partner}, device_id_type=MESH,
            ).wait_recv()
            values = att_in[s].astype(F32)
        else:
            values = att_out[i].astype(F32)
        at = pl.ds(pl.multiple_of(s * group, group), group)
        square = jnp.sum(values * values, axis=-1, keepdims=True)
        squares = square if squares is None else squares + square
        scaled = (values * og_ref[s].astype(F32)).astype(BF16)
        term = jnp.dot(scaled, wout[at, :], preferred_element_type=F32)
        if t == 0:
            acc[...] = term
        elif t < n - 1:
            acc[...] += term
        else:
            factor = lax.rsqrt(squares / (n * group) + 1e-05)
            out_ref[0] = ((acc[...] + term) * factor).astype(BF16)

    for copy in sends:
        copy.wait_send()
    for event in events:
        relay_finish(*event)
    for b in range(n):
        @pl.when(i != b)
        def _(b=b):
            att_copy(b).wait_send()


def x_size(mesh):
    row = mesh.devices[0]
    places = [getattr(device, "coords", None) for device in row]
    if any(place is None for place in places):
        return 1
    return len({place[0] for place in places})


def per_device(
    mesh, q_latent, kv_latent, rope_key, w_query, w_keyval, w_out, query_gain, latent_gain, out_gain
):
    n, m = mesh.shape["sp"], mesh.shape["dp"]
    rows = q_latent.shape[1]
    length = n * rows
    rank = q_latent.shape[2]
    width = w_query.shape[1]
    local_heads = H // n
    k = local_heads * HEAD // width
    chunks = 8
    dim = w_out.shape[1]
    group = local_heads * VDIM
    table = jnp.asarray(turn_table(length))
    geometry = (n, m, x_size(mesh), k, chunks, local_heads)
    any_spec = pl.BlockSpec(memory_space=pl.ANY)
    vmem_spec = pl.BlockSpec(memory_space=pltpu.VMEM)
    dma = pltpu.SemaphoreType.DMA
    return pl.pallas_call(
        functools.partial(kernel, geometry),
        out_shape=jax.ShapeDtypeStruct((1, rows, dim), BF16),
        in_specs=[any_spec] * 7 + [vmem_spec] * 3,
        out_specs=vmem_spec,
        scratch_shapes=[
            pltpu.VMEM((n, rows, rank), BF16),
            pltpu.VMEM((n, rows, kv_latent.shape[2]), BF16),
            pltpu.VMEM((n, rows, ROPE), BF16),
            pltpu.VMEM((k, rank, width), BF16),
            pltpu.VMEM(w_keyval.shape, BF16),
            pltpu.VMEM(w_out.shape, BF16),
            pltpu.VMEM((length, 128), F32),
            pltpu.VMEM((local_heads, rank, 256), BF16),
            pltpu.VMEM((length, rank), BF16),
            pltpu.VMEM((local_heads, length, 256), BF16),
            pltpu.VMEM((local_heads, length, 256), BF16),
            pltpu.VMEM((local_heads, length, VDIM), BF16),
            pltpu.VMEM((n, rows, group), BF16),
            pltpu.VMEM((n, rows, group), BF16),
            pltpu.VMEM((rows, dim), F32),
            dma((7,)),
            dma((3, n // 2)),
            dma((3, n)),
            dma((3, n // 2)),
            dma((4, k, chunks)),
            dma((k, chunks)),
            dma((n,)),
            dma((n,)),
        ],
        compiler_params=pltpu.CompilerParams(
            collective_id=0, has_side_effects=True, vmem_limit_bytes=56 * 1024 * 1024
        ),
    )(
        q_latent, kv_latent, rope_key, w_query, w_keyval, w_out, table,
        query_gain.reshape(1, -1), latent_gain.reshape(1, -1),
        out_gain.reshape(n, 1, group),
    )


def solution(mesh):
    in_specs = (
        P("dp", "sp", None),
        P("dp", "sp", None),
        P("dp", "sp", None),
        P(None, "dp"),
        P(None, "sp"),
        P(),
        P(),
        P(),
        P(),
    )
    return jax.shard_map(
        functools.partial(per_device, mesh), mesh=mesh, in_specs=in_specs,
        out_specs=P("dp", "sp", None), check_vma=False,
    )
```

```python
import functools

import jax
import jax.numpy as jnp
import numpy as np
from jax import lax
from jax.experimental import pallas as pl
from jax.experimental.pallas import tpu as pltpu
from jax.sharding import PartitionSpec as P

H = 16
NOPE = 128
ROPE = 64
VDIM = 128
HEAD = NOPE + ROPE
MESH = pl.DeviceIdType.MESH
F32 = jnp.float32
BF16 = jnp.bfloat16


def turn_table(length):
    half = ROPE // 2
    inverse = np.float32(10000.0) ** (-np.arange(half, dtype=np.float32) / np.float32(half))
    angles = np.arange(length, dtype=np.float32)[:, None] * inverse[None, :].astype(np.float32)
    angles = angles.astype(np.float64)
    cosine, sine = np.cos(angles), np.sin(angles)
    return np.concatenate([cosine, cosine, sine, sine], axis=1).astype(np.float32)


def spread_matrix(rows, row_start, head):
    g = lax.broadcasted_iota(jnp.int32, (rows, 256), 0) + row_start
    f = lax.broadcasted_iota(jnp.int32, (rows, 256), 1)
    source = jnp.where(f < HEAD, f, jnp.where(f < HEAD + 32, f - 32, f - 96)) + head * HEAD
    sign = jnp.where((f >= HEAD) & (f < HEAD + 32), -1.0, 1.0)
    return jnp.where(g == source, sign, 0.0).astype(BF16)


def rope_matrix():
    r = lax.broadcasted_iota(jnp.int32, (ROPE, 128), 0)
    f = lax.broadcasted_iota(jnp.int32, (ROPE, 128), 1)
    source = jnp.where(f < 64, f, jnp.where(f < 96, f - 32, f - 96))
    sign = jnp.where((f >= 64) & (f < 96), -1.0, 1.0)
    return jnp.where(r == source, sign, 0.0).astype(BF16)


def scaled_rows(values, gain):
    wide = values.astype(F32)
    mean = jnp.mean(wide * wide, axis=-1, keepdims=True)
    return (wide * lax.rsqrt(mean + 1e-05) * gain).astype(BF16)


def kernel(
    geometry,
    q_ref, kv_ref, rope_ref, wq_ref, wkv_ref, wout_ref, table_ref, qg_ref, lg_ref, og_ref,
    out_ref,
    qall, kvall, ropeall, wqall, wkv, wout, table, spread, qn, qs, ks, vs, att_out, att_in, acc,
    out_gain,
    local_sem, gat_send, gat_recv, fwd_send, w_send, w_recv, att_send, att_recv,
):
    n, m, X, k, chunks, local_heads, groups = geometry
    per_group = local_heads // groups
    width = wqall.shape[2]
    Z = m // X
    rows = q_ref.shape[1]
    n_chips = n // 2
    i = lax.axis_index("sp")
    j = lax.axis_index("dp")
    core = lax.rem(i, 2)
    chip = lax.div(i, 2)
    partner = i + 1 - 2 * core
    z = lax.div(j, X)
    x = lax.rem(j, X)
    first = i * k
    owns = (j >= first) & (j < first + k)

    gathered = ((kv_ref.at[0], kvall), (rope_ref.at[0], ropeall), (q_ref.at[0], qall))
    own_copies = [
        pltpu.make_async_copy(src, dst.at[i], local_sem.at[a]) for a, (src, dst) in enumerate(gathered)
    ]
    wq_copy = pltpu.make_async_copy(wq_ref, wqall.at[lax.rem(j, k)], local_sem.at[3])
    wkv_copy = pltpu.make_async_copy(wkv_ref, wkv, local_sem.at[4])
    table_copy = pltpu.make_async_copy(table_ref, table, local_sem.at[5])
    wout_copy = pltpu.make_async_copy(wout_ref, wout, local_sem.at[6])

    @pl.when(owns)
    def _():
        wq_copy.start()

    for copy in own_copies:
        copy.start()
    wkv_copy.start()
    table_copy.start()
    wout_copy.start()

    turner = rope_matrix()
    latent_gain = lg_ref[...].astype(F32).reshape(1, -1)
    query_gain = qg_ref[...].astype(F32).reshape(1, -1)
    group = local_heads * VDIM
    every_gain = og_ref[...].astype(F32).reshape(1, -1)
    for s in range(n):
        out_gain[s] = every_gain[:, s * group:(s + 1) * group]
    if groups > 1:
        for h in range(per_group):
            spread[h] = spread_matrix(width, 0, h)

    barrier = pltpu.get_barrier_semaphore()
    for d in range(1, n):
        pl.semaphore_signal(
            barrier, inc=1, device_id={"sp": lax.rem(i + d, n)}, device_id_type=MESH
        )
    sides = ((z < Z - 1, j + X), (z > 0, j - X), (x < X - 1, j + 1), (x > 0, j - 1))
    count = n - 1
    for present, target in sides:
        @pl.when(present)
        def _(target=target):
            pl.semaphore_signal(barrier, inc=1, device_id={"dp": target}, device_id_type=MESH)
        count = count + jnp.where(present, 1, 0)
    pl.semaphore_wait(barrier, count)

    step_rows = wqall.shape[1] // chunks

    def relay_parts(slot, c):
        owner = first + slot
        zo, xo = lax.div(owner, X), lax.rem(owner, X)
        part = wqall.at[slot, pl.ds(c * step_rows, step_rows)]
        in_column = x == xo
        conditions = (
            in_column & (z >= zo) & (z < Z - 1),
            in_column & (z <= zo) & (z > 0),
            (x >= xo) & (x < X - 1),
            (x <= xo) & (x > 0),
        )
        copies = [
            pltpu.make_async_remote_copy(
                src_ref=part, dst_ref=part,
                send_sem=w_send.at[side, slot, c], recv_sem=w_recv.at[slot, c],
                device_id={"dp": sides[side][1]}, device_id_type=MESH,
            )
            for side in range(4)
        ]
        return owner, conditions, copies

    def relay(slot, c):
        owner, conditions, copies = relay_parts(slot, c)

        @pl.when(owner != j)
        def _():
            copies[0].wait_recv()

        for condition, copy in zip(conditions, copies):
            @pl.when(condition)
            def _(copy=copy):
                copy.start()

    def relay_finish(slot, c):
        _, conditions, copies = relay_parts(slot, c)
        for condition, copy in zip(conditions, copies):
            @pl.when(condition)
            def _(copy=copy):
                copy.wait_send()

    if groups > 1:
        columns = [lax.rem(x + t, k) for t in range(k)]
        events = [[(column, c) for c in range(chunks)] for column in columns]
    else:
        columns = [0]
        events = [[(slot, c) for c in range(chunks) for slot in range(k)]]
    events_left = list(events[0])

    def relay_some(number):
        for _ in range(min(number, len(events_left))):
            relay(*events_left.pop(0))

    def gather_copy(a, slot, sem, target):
        dst = gathered[a][1]
        return pltpu.make_async_remote_copy(
            src_ref=dst.at[slot], dst_ref=dst.at[slot],
            send_sem=sem, recv_sem=gat_recv.at[a, slot],
            device_id={"sp": target}, device_id_type=MESH,
        )

    sends = []

    @pl.when(owns)
    def _():
        wq_copy.wait()

    for a in range(3):
        own_copies[a].wait()
        for d in range(1, n_chips):
            target = 2 * lax.rem(chip + d, n_chips) + core
            sends.append(gather_copy(a, i, gat_send.at[a, d], target))
            sends[-1].start()
    for a in range(3):
        sends.append(gather_copy(a, i, gat_send.at[a, 0], partner))
        sends[-1].start()

    def far_slot(d):
        return 2 * lax.rem(chip + n_chips - d, n_chips) + core

    def forward(a, d):
        slot = far_slot(d)
        copy = gather_copy(a, slot, fwd_send.at[a, d - 1], partner)
        copy.wait_recv()
        copy.start()
        sends.append(copy)

    def arrive(a, slot):
        gather_copy(a, slot, gat_send.at[a, 0], partner).wait_recv()

    lane = lax.broadcasted_iota(jnp.int32, (rows, 128), 1)

    def keyval(slot):
        at = pl.ds(pl.multiple_of(slot * rows, rows), rows)
        both = jnp.dot(
            scaled_rows(kvall[slot], latent_gain), wkv[...], preferred_element_type=F32
        ).astype(BF16)
        pair = lax.dot_general(
            ropeall[slot], turner, (((0,), (0,)), ((), ())), preferred_element_type=F32
        ) * table[at, :]
        pair = pair + pltpu.roll(pair, 64, 1)
        turned = jnp.where(lane < 64, pair, 0.0).astype(BF16)
        for h in range(local_heads):
            base = h * (NOPE + VDIM)
            ks[h, at, 0:NOPE] = both[:, base:base + NOPE]
            ks[h, at, NOPE:256] = turned
            vs[h, at, :] = both[:, base + NOPE:base + NOPE + VDIM]

    def query_rows(slot):
        at = pl.ds(pl.multiple_of(slot * rows, rows), rows)
        qn[at, :] = scaled_rows(qall[slot], query_gain)

    relay_some(k + 1)
    wkv_copy.wait()
    table_copy.wait()
    keyval(i)
    relay_some(1)
    query_rows(i)
    relay_some(1)
    arrive(0, partner)
    arrive(1, partner)
    keyval(partner)
    relay_some(1)
    for d in range(1, n_chips):
        forward(0, d)
        forward(1, d)
        keyval(far_slot(d))
        relay_some(1)
    arrive(2, partner)
    query_rows(partner)
    relay_some(2)
    for d in range(1, n_chips):
        other = far_slot(d) + 1 - 2 * core
        arrive(0, other)
        arrive(1, other)
        keyval(other)
        relay_some(2)
    for d in range(1, n_chips):
        forward(2, d)
        query_rows(far_slot(d))
        relay_some(2)
    for d in range(1, n_chips):
        other = far_slot(d) + 1 - 2 * core
        arrive(2, other)
        query_rows(other)
    relay_some(len(events_left))

    def raw_queries(slot, hh):
        if groups > 1:
            total = jnp.dot(wqall[slot], spread[hh], preferred_element_type=F32)
        else:
            total = None
            for s in range(k):
                if (s + 1) * width <= hh * HEAD or s * width >= (hh + 1) * HEAD:
                    continue
                term = jnp.dot(
                    wqall[s], spread_matrix(width, s * width, hh), preferred_element_type=F32
                )
                total = term if total is None else total + term
        return jnp.dot(qn[...], total.astype(BF16), preferred_element_type=F32)

    def queries(slot):
        for hh in range(per_group):
            h = slot * per_group + hh
            raw = raw_queries(slot, hh)
            qs[h, :, 0:NOPE] = raw[:, 0:NOPE].astype(BF16)
            pair = raw[:, NOPE:256] * table[...]
            qs[h, :, NOPE:256] = (pair + pltpu.roll(pair, 64, 1)).astype(BF16)

    power = HEAD ** (-0.5) * float(np.log2(np.e))
    causal = lax.broadcasted_iota(jnp.int32, (rows, rows), 1) <= lax.broadcasted_iota(
        jnp.int32, (rows, rows), 0
    )

    def attend(b, slot):
        stop = (b + 1) * rows
        for hh in range(per_group):
            h = slot * per_group + hh
            scores = lax.dot_general(
                qs[h, b * rows:stop, :], ks[h, 0:stop, :], (((1,), (1,)), ((), ())),
                preferred_element_type=F32,
            )
            last = jnp.where(causal, scores[:, b * rows:], -jnp.inf)
            if b:
                scores = jnp.concatenate([scores[:, :b * rows], last], axis=1)
            else:
                scores = last
            top = jnp.max(scores, axis=-1, keepdims=True)
            weights = jnp.exp2((scores - top) * power)
            row_total = jnp.sum(weights, axis=-1, keepdims=True)
            summed = jnp.dot(weights.astype(BF16), vs[h, 0:stop, :], preferred_element_type=F32)
            att_out[b, slot, :, hh * VDIM:(hh + 1) * VDIM] = (summed / row_total).astype(BF16)

    def att_copy(b, slot):
        return pltpu.make_async_remote_copy(
            src_ref=att_out.at[b, slot], dst_ref=att_in.at[i, slot],
            send_sem=att_send.at[b, slot], recv_sem=att_recv.at[i, slot],
            device_id={"sp": b}, device_id_type=MESH,
        )

    for t, slot in enumerate(columns):
        if t:
            for event in events[t]:
                relay(*event)
        queries(slot)
        for b in range(n):
            @pl.when(chip != b // 2)
            def _(b=b):
                attend(b, slot)
                att_copy(b, slot).start()
        for b in range(n):
            @pl.when(partner == b)
            def _(b=b):
                attend(b, slot)
                att_copy(b, slot).start()
        for b in range(n):
            @pl.when(i == b)
            def _(b=b):
                attend(b, slot)

    wout_copy.wait()
    squares = None
    order = [partner]
    for d in range(1, n_chips):
        order += [far_slot(d), far_slot(d) + 1 - 2 * core]
    for t, s in enumerate([i] + order):
        source = att_out
        if t:
            source = att_in
            for slot in range(groups):
                pltpu.make_async_remote_copy(
                    src_ref=att_in.at[s, slot], dst_ref=att_in.at[s, slot],
                    send_sem=att_send.at[0, slot], recv_sem=att_recv.at[s, slot],
                    device_id={"sp": partner}, device_id_type=MESH,
                ).wait_recv()
        values = jnp.concatenate([source[s, slot] for slot in range(groups)], axis=1).astype(F32)
        at = pl.ds(pl.multiple_of(s * group, group), group)
        square = jnp.sum(values * values, axis=-1, keepdims=True)
        squares = square if squares is None else squares + square
        scaled = (values * out_gain[s]).astype(BF16)
        term = jnp.dot(scaled, wout[at, :], preferred_element_type=F32)
        if t == 0:
            acc[...] = term
        elif t < n - 1:
            acc[...] += term
        else:
            factor = lax.rsqrt(squares / (n * group) + 1e-05)
            out_ref[0] = ((acc[...] + term) * factor).astype(BF16)

    for copy in sends:
        copy.wait_send()
    for event in sum(events, []):
        relay_finish(*event)
    for b in range(n):
        @pl.when(i != b)
        def _(b=b):
            for slot in range(groups):
                att_copy(b, slot).wait_send()


def x_size(mesh):
    row = mesh.devices[0]
    places = [getattr(device, "coords", None) for device in row]
    if any(place is None for place in places):
        return 1
    return len({place[0] for place in places})


def per_device(
    mesh, q_latent, kv_latent, rope_key, w_query, w_keyval, w_out, query_gain, latent_gain, out_gain
):
    n, m = mesh.shape["sp"], mesh.shape["dp"]
    rows = q_latent.shape[1]
    length = n * rows
    rank = q_latent.shape[2]
    width = w_query.shape[1]
    local_heads = H // n
    k = local_heads * HEAD // width
    chunks = 16
    columns = x_size(mesh)
    groups = k if k == columns == 2 and width % HEAD == 0 else 1
    dim = w_out.shape[1]
    group = local_heads * VDIM
    table = jnp.asarray(turn_table(length))
    geometry = (n, m, columns, k, chunks, local_heads, groups)
    any_spec = pl.BlockSpec(memory_space=pl.ANY)
    vmem_spec = pl.BlockSpec(memory_space=pltpu.VMEM)
    dma = pltpu.SemaphoreType.DMA
    return pl.pallas_call(
        functools.partial(kernel, geometry),
        out_shape=jax.ShapeDtypeStruct((1, rows, dim), BF16),
        in_specs=[any_spec] * 7 + [vmem_spec] * 3,
        out_specs=vmem_spec,
        scratch_shapes=[
            pltpu.VMEM((n, rows, rank), BF16),
            pltpu.VMEM((n, rows, kv_latent.shape[2]), BF16),
            pltpu.VMEM((n, ROPE, rows), BF16),
            pltpu.VMEM((k, rank, width), BF16),
            pltpu.VMEM(w_keyval.shape, BF16),
            pltpu.VMEM(w_out.shape, BF16),
            pltpu.VMEM((length, 128), F32),
            pltpu.VMEM((local_heads // groups, width, 256), BF16),
            pltpu.VMEM((length, rank), BF16),
            pltpu.VMEM((local_heads, length, 256), BF16),
            pltpu.VMEM((local_heads, length, 256), BF16),
            pltpu.VMEM((local_heads, length, VDIM), BF16),
            pltpu.VMEM((n, groups, rows, group // groups), BF16),
            pltpu.VMEM((n, groups, rows, group // groups), BF16),
            pltpu.VMEM((rows, dim), F32),
            pltpu.VMEM((n, 1, group), F32),
            dma((7,)),
            dma((3, n // 2)),
            dma((3, n)),
            dma((3, n // 2)),
            dma((4, k, chunks)),
            dma((k, chunks)),
            dma((n, groups)),
            dma((n, groups)),
        ],
        compiler_params=pltpu.CompilerParams(
            collective_id=0, has_side_effects=True, vmem_limit_bytes=56 * 1024 * 1024
        ),
    )(
        q_latent, kv_latent, jnp.swapaxes(rope_key, 1, 2), w_query, w_keyval, w_out, table,
        query_gain, latent_gain, out_gain,
    )


def solution(mesh):
    in_specs = (
        P("dp", "sp", None),
        P("dp", "sp", None),
        P("dp", "sp", None),
        P(None, "dp"),
        P(None, "sp"),
        P(),
        P(),
        P(),
        P(),
    )
    return jax.shard_map(
        functools.partial(per_device, mesh), mesh=mesh, in_specs=in_specs,
        out_specs=P("dp", "sp", None), check_vma=False,
    )
```

```python
import functools

import jax
import jax.numpy as jnp
import numpy as np
from jax import lax
from jax.experimental import pallas as pl
from jax.experimental.pallas import tpu as pltpu
from jax.sharding import PartitionSpec as P

H = 16
NOPE = 128
ROPE = 64
VDIM = 128
HEAD = NOPE + ROPE
MESH = pl.DeviceIdType.MESH
F32 = jnp.float32
BF16 = jnp.bfloat16


def turn_table(length):
    half = ROPE // 2
    inverse = np.float32(10000.0) ** (-np.arange(half, dtype=np.float32) / np.float32(half))
    angles = np.arange(length, dtype=np.float32)[:, None] * inverse[None, :].astype(np.float32)
    angles = angles.astype(np.float64)
    cosine, sine = np.cos(angles), np.sin(angles)
    return np.concatenate([cosine, cosine, sine, sine], axis=1).astype(np.float32)


def spread_matrix(rows, row_start, head):
    g = lax.broadcasted_iota(jnp.int32, (rows, 256), 0) + row_start
    f = lax.broadcasted_iota(jnp.int32, (rows, 256), 1)
    source = jnp.where(f < HEAD, f, jnp.where(f < HEAD + 32, f - 32, f - 96)) + head * HEAD
    sign = jnp.where((f >= HEAD) & (f < HEAD + 32), -1.0, 1.0)
    return jnp.where(g == source, sign, 0.0).astype(BF16)


def rope_matrix():
    r = lax.broadcasted_iota(jnp.int32, (ROPE, 128), 0)
    f = lax.broadcasted_iota(jnp.int32, (ROPE, 128), 1)
    source = jnp.where(f < 64, f, jnp.where(f < 96, f - 32, f - 96))
    sign = jnp.where((f >= 64) & (f < 96), -1.0, 1.0)
    return jnp.where(r == source, sign, 0.0).astype(BF16)


def scaled_rows(values, gain):
    wide = values.astype(F32)
    mean = jnp.mean(wide * wide, axis=-1, keepdims=True)
    return (wide * lax.rsqrt(mean + 1e-05) * gain).astype(BF16)


def kernel(
    geometry,
    q_ref, kv_ref, rope_ref, wq_ref, wkv_ref, wout_ref, table_ref, qg_ref, lg_ref, og_ref,
    out_ref,
    qall, kvall, ropeall, wqall, wkv, wout, table, spread, qn, qs, ks, vs, att_out, att_in, acc,
    out_gain,
    local_sem, gat_send, gat_recv, fwd_send, w_send, w_recv, att_send, att_recv,
):
    n, m, X, k, chunks, local_heads, groups = geometry
    per_group = local_heads // groups
    width = wqall.shape[2]
    Z = m // X
    rows = q_ref.shape[1]
    n_chips = n // 2
    i = lax.axis_index("sp")
    j = lax.axis_index("dp")
    core = lax.rem(i, 2)
    chip = lax.div(i, 2)
    partner = i + 1 - 2 * core
    z = lax.div(j, X)
    x = lax.rem(j, X)
    first = i * k
    owns = (j >= first) & (j < first + k)

    gathered = ((kv_ref.at[0], kvall), (rope_ref.at[0], ropeall), (q_ref.at[0], qall))
    own_copies = [
        pltpu.make_async_copy(src, dst.at[i], local_sem.at[a]) for a, (src, dst) in enumerate(gathered)
    ]
    wq_copy = pltpu.make_async_copy(wq_ref, wqall.at[lax.rem(j, k)], local_sem.at[3])
    wkv_copy = pltpu.make_async_copy(wkv_ref, wkv, local_sem.at[4])
    table_copy = pltpu.make_async_copy(table_ref, table, local_sem.at[5])
    wout_copy = pltpu.make_async_copy(wout_ref, wout, local_sem.at[6])

    @pl.when(owns)
    def _():
        wq_copy.start()

    for copy in own_copies:
        copy.start()
    wkv_copy.start()
    table_copy.start()
    wout_copy.start()

    turner = rope_matrix()
    latent_gain = lg_ref[...].astype(F32).reshape(1, -1)
    query_gain = qg_ref[...].astype(F32).reshape(1, -1)
    group = local_heads * VDIM
    every_gain = og_ref[...].astype(F32).reshape(1, -1)
    for s in range(n):
        out_gain[s] = every_gain[:, s * group:(s + 1) * group]
    if groups > 1:
        for h in range(per_group):
            spread[h] = spread_matrix(width, 0, h)

    barrier = pltpu.get_barrier_semaphore()
    for d in range(1, n):
        pl.semaphore_signal(
            barrier, inc=1, device_id={"sp": lax.rem(i + d, n)}, device_id_type=MESH
        )
    sides = ((z < Z - 1, j + X), (z > 0, j - X), (x < X - 1, j + 1), (x > 0, j - 1))
    count = n - 1
    for present, target in sides:
        @pl.when(present)
        def _(target=target):
            pl.semaphore_signal(barrier, inc=1, device_id={"dp": target}, device_id_type=MESH)
        count = count + jnp.where(present, 1, 0)
    pl.semaphore_wait(barrier, count)

    step_rows = wqall.shape[1] // chunks

    def relay_parts(slot, c):
        owner = first + slot
        zo, xo = lax.div(owner, X), lax.rem(owner, X)
        part = wqall.at[slot, pl.ds(c * step_rows, step_rows)]
        in_column = x == xo
        conditions = (
            in_column & (z >= zo) & (z < Z - 1),
            in_column & (z <= zo) & (z > 0),
            (x >= xo) & (x < X - 1),
            (x <= xo) & (x > 0),
        )
        copies = [
            pltpu.make_async_remote_copy(
                src_ref=part, dst_ref=part,
                send_sem=w_send.at[side, slot, c], recv_sem=w_recv.at[slot, c],
                device_id={"dp": sides[side][1]}, device_id_type=MESH,
            )
            for side in range(4)
        ]
        return owner, conditions, copies

    def relay(slot, c):
        owner, conditions, copies = relay_parts(slot, c)

        @pl.when(owner != j)
        def _():
            copies[0].wait_recv()

        for condition, copy in zip(conditions, copies):
            @pl.when(condition)
            def _(copy=copy):
                copy.start()

    def relay_finish(slot, c):
        _, conditions, copies = relay_parts(slot, c)
        for condition, copy in zip(conditions, copies):
            @pl.when(condition)
            def _(copy=copy):
                copy.wait_send()

    if groups > 1:
        columns = [lax.rem(x + t, k) for t in range(k)]
        events = [[(column, c) for c in range(chunks)] for column in columns]
    else:
        columns = [0]
        events = [[(slot, c) for c in range(chunks) for slot in range(k)]]
    events_left = list(events[0])

    def relay_some(number):
        for _ in range(min(number, len(events_left))):
            relay(*events_left.pop(0))

    def gather_copy(a, slot, sem, target):
        dst = gathered[a][1]
        return pltpu.make_async_remote_copy(
            src_ref=dst.at[slot], dst_ref=dst.at[slot],
            send_sem=sem, recv_sem=gat_recv.at[a, slot],
            device_id={"sp": target}, device_id_type=MESH,
        )

    sends = []

    @pl.when(owns)
    def _():
        wq_copy.wait()

    for a in range(3):
        own_copies[a].wait()
        for d in range(1, n_chips):
            target = 2 * lax.rem(chip + d, n_chips) + core
            sends.append(gather_copy(a, i, gat_send.at[a, d], target))
            sends[-1].start()
    for a in range(3):
        sends.append(gather_copy(a, i, gat_send.at[a, 0], partner))
        sends[-1].start()

    def far_slot(d):
        return 2 * lax.rem(chip + n_chips - d, n_chips) + core

    def forward(a, d):
        slot = far_slot(d)
        copy = gather_copy(a, slot, fwd_send.at[a, d - 1], partner)
        copy.wait_recv()
        copy.start()
        sends.append(copy)

    def arrive(a, slot):
        gather_copy(a, slot, gat_send.at[a, 0], partner).wait_recv()

    lane = lax.broadcasted_iota(jnp.int32, (rows, 128), 1)

    def keyval(slot):
        at = pl.ds(pl.multiple_of(slot * rows, rows), rows)
        both = jnp.dot(
            scaled_rows(kvall[slot], latent_gain), wkv[...], preferred_element_type=F32
        ).astype(BF16)
        pair = lax.dot_general(
            ropeall[slot], turner, (((0,), (0,)), ((), ())), preferred_element_type=F32
        ) * table[at, :]
        pair = pair + pltpu.roll(pair, 64, 1)
        turned = jnp.where(lane < 64, pair, 0.0).astype(BF16)
        for h in range(local_heads):
            base = h * (NOPE + VDIM)
            ks[h, at, 0:NOPE] = both[:, base:base + NOPE]
            ks[h, at, NOPE:256] = turned
            vs[h, at, :] = both[:, base + NOPE:base + NOPE + VDIM]

    def query_rows(slot):
        at = pl.ds(pl.multiple_of(slot * rows, rows), rows)
        qn[at, :] = scaled_rows(qall[slot], query_gain)

    relay_some(k + 1)
    wkv_copy.wait()
    table_copy.wait()
    keyval(i)
    relay_some(1)
    query_rows(i)
    relay_some(1)
    arrive(0, partner)
    arrive(1, partner)
    keyval(partner)
    relay_some(1)
    for d in range(1, n_chips):
        forward(0, d)
        forward(1, d)
        keyval(far_slot(d))
        relay_some(1)
    arrive(2, partner)
    query_rows(partner)
    relay_some(2)
    for d in range(1, n_chips):
        other = far_slot(d) + 1 - 2 * core
        arrive(0, other)
        arrive(1, other)
        keyval(other)
        relay_some(2)
    for d in range(1, n_chips):
        forward(2, d)
        query_rows(far_slot(d))
        relay_some(2)
    for d in range(1, n_chips):
        other = far_slot(d) + 1 - 2 * core
        arrive(2, other)
        query_rows(other)
    relay_some(len(events_left))

    def raw_queries(slot, hh):
        if groups > 1:
            total = jnp.dot(wqall[slot], spread[hh], preferred_element_type=F32)
        else:
            total = None
            for s in range(k):
                if (s + 1) * width <= hh * HEAD or s * width >= (hh + 1) * HEAD:
                    continue
                term = jnp.dot(
                    wqall[s], spread_matrix(width, s * width, hh), preferred_element_type=F32
                )
                total = term if total is None else total + term
        return jnp.dot(qn[...], total.astype(BF16), preferred_element_type=F32)

    def queries(slot):
        for hh in range(per_group):
            h = slot * per_group + hh
            raw = raw_queries(slot, hh)
            qs[h, :, 0:NOPE] = raw[:, 0:NOPE].astype(BF16)
            pair = raw[:, NOPE:256] * table[...]
            qs[h, :, NOPE:256] = (pair + pltpu.roll(pair, 64, 1)).astype(BF16)

    power = HEAD ** (-0.5) * float(np.log2(np.e))
    causal = lax.broadcasted_iota(jnp.int32, (rows, rows), 1) <= lax.broadcasted_iota(
        jnp.int32, (rows, rows), 0
    )

    def attend(b, slot):
        stop = (b + 1) * rows
        for hh in range(per_group):
            h = slot * per_group + hh
            scores = lax.dot_general(
                qs[h, b * rows:stop, :], ks[h, 0:stop, :], (((1,), (1,)), ((), ())),
                preferred_element_type=F32,
            )
            last = jnp.where(causal, scores[:, b * rows:], -jnp.inf)
            if b:
                scores = jnp.concatenate([scores[:, :b * rows], last], axis=1)
            else:
                scores = last
            top = jnp.max(scores, axis=-1, keepdims=True)
            weights = jnp.exp2((scores - top) * power)
            row_total = jnp.sum(weights, axis=-1, keepdims=True)
            summed = jnp.dot(weights.astype(BF16), vs[h, 0:stop, :], preferred_element_type=F32)
            att_out[b, slot, :, hh * VDIM:(hh + 1) * VDIM] = (summed / row_total).astype(BF16)

    def att_copy(b, slot):
        return pltpu.make_async_remote_copy(
            src_ref=att_out.at[b, slot], dst_ref=att_in.at[i, slot],
            send_sem=att_send.at[b, slot], recv_sem=att_recv.at[i, slot],
            device_id={"sp": b}, device_id_type=MESH,
        )

    for t, slot in enumerate(columns):
        if t:
            for event in events[t]:
                relay(*event)
        queries(slot)
        for c in range(n_chips):
            @pl.when(chip != c)
            def _(c=c):
                for b in (2 * c, 2 * c + 1):
                    attend(b, slot)
                    att_copy(b, slot).start()
    for c in range(n_chips):
        @pl.when(chip == c)
        def _(c=c):
            for slot in columns:
                for b in (2 * c, 2 * c + 1):
                    attend(b, slot)
    for slot in columns:
        att_copy(partner, slot).start()

    wout_copy.wait()
    squares = None
    order = [partner]
    for d in range(1, n_chips):
        order += [far_slot(d), far_slot(d) + 1 - 2 * core]
    for t, s in enumerate([i] + order):
        source = att_out
        if t:
            source = att_in
            for slot in range(groups):
                pltpu.make_async_remote_copy(
                    src_ref=att_in.at[s, slot], dst_ref=att_in.at[s, slot],
                    send_sem=att_send.at[0, slot], recv_sem=att_recv.at[s, slot],
                    device_id={"sp": partner}, device_id_type=MESH,
                ).wait_recv()
        values = jnp.concatenate([source[s, slot] for slot in range(groups)], axis=1).astype(F32)
        at = pl.ds(pl.multiple_of(s * group, group), group)
        square = jnp.sum(values * values, axis=-1, keepdims=True)
        squares = square if squares is None else squares + square
        scaled = (values * out_gain[s]).astype(BF16)
        term = jnp.dot(scaled, wout[at, :], preferred_element_type=F32)
        if t == 0:
            acc[...] = term
        elif t < n - 1:
            acc[...] += term
        else:
            factor = lax.rsqrt(squares / (n * group) + 1e-05)
            out_ref[0] = ((acc[...] + term) * factor).astype(BF16)

    for copy in sends:
        copy.wait_send()
    for event in sum(events, []):
        relay_finish(*event)
    for b in range(n):
        @pl.when(i != b)
        def _(b=b):
            for slot in range(groups):
                att_copy(b, slot).wait_send()


def x_size(mesh):
    row = mesh.devices[0]
    places = [getattr(device, "coords", None) for device in row]
    if any(place is None for place in places):
        return 1
    return len({place[0] for place in places})


def per_device(
    mesh, q_latent, kv_latent, rope_key, w_query, w_keyval, w_out, query_gain, latent_gain, out_gain
):
    n, m = mesh.shape["sp"], mesh.shape["dp"]
    rows = q_latent.shape[1]
    length = n * rows
    rank = q_latent.shape[2]
    width = w_query.shape[1]
    local_heads = H // n
    k = local_heads * HEAD // width
    chunks = 16
    columns = x_size(mesh)
    groups = k if k == columns == 2 and width % HEAD == 0 else 1
    dim = w_out.shape[1]
    group = local_heads * VDIM
    table = jnp.asarray(turn_table(length))
    geometry = (n, m, columns, k, chunks, local_heads, groups)
    any_spec = pl.BlockSpec(memory_space=pl.ANY)
    vmem_spec = pl.BlockSpec(memory_space=pltpu.VMEM)
    dma = pltpu.SemaphoreType.DMA
    return pl.pallas_call(
        functools.partial(kernel, geometry),
        out_shape=jax.ShapeDtypeStruct((1, rows, dim), BF16),
        in_specs=[any_spec] * 7 + [vmem_spec] * 3,
        out_specs=vmem_spec,
        scratch_shapes=[
            pltpu.VMEM((n, rows, rank), BF16),
            pltpu.VMEM((n, rows, kv_latent.shape[2]), BF16),
            pltpu.VMEM((n, ROPE, rows), BF16),
            pltpu.VMEM((k, rank, width), BF16),
            pltpu.VMEM(w_keyval.shape, BF16),
            pltpu.VMEM(w_out.shape, BF16),
            pltpu.VMEM((length, 128), F32),
            pltpu.VMEM((local_heads // groups, width, 256), BF16),
            pltpu.VMEM((length, rank), BF16),
            pltpu.VMEM((local_heads, length, 256), BF16),
            pltpu.VMEM((local_heads, length, 256), BF16),
            pltpu.VMEM((local_heads, length, VDIM), BF16),
            pltpu.VMEM((n, groups, rows, group // groups), BF16),
            pltpu.VMEM((n, groups, rows, group // groups), BF16),
            pltpu.VMEM((rows, dim), F32),
            pltpu.VMEM((n, 1, group), F32),
            dma((7,)),
            dma((3, n // 2)),
            dma((3, n)),
            dma((3, n // 2)),
            dma((4, k, chunks)),
            dma((k, chunks)),
            dma((n, groups)),
            dma((n, groups)),
        ],
        compiler_params=pltpu.CompilerParams(
            collective_id=0, has_side_effects=True, vmem_limit_bytes=56 * 1024 * 1024
        ),
    )(
        q_latent, kv_latent, jnp.swapaxes(rope_key, 1, 2), w_query, w_keyval, w_out, table,
        query_gain, latent_gain, out_gain,
    )


def solution(mesh):
    in_specs = (
        P("dp", "sp", None),
        P("dp", "sp", None),
        P("dp", "sp", None),
        P(None, "dp"),
        P(None, "sp"),
        P(),
        P(),
        P(),
        P(),
    )
    return jax.shard_map(
        functools.partial(per_device, mesh), mesh=mesh, in_specs=in_specs,
        out_specs=P("dp", "sp", None), check_vma=False,
    )
```
